512 devices in a mesh: ep: 32 (over z, core), tp: 16 (over y, x).
Axes of the slice: x: 4, y: 4, z: 16, core: 2. Of those that a mesh axis runs over, the one named last changes fastest.
Arguments:
- tokens: bfloat16 [8192, 2048], P('ep', 'tp'), may hold values from -800 to 800
- norm_gain: bfloat16 [2048], P('tp'), may hold values from 0.099609375 to 1.8984375
- w_gate: bfloat16 [32, 2048, 6144], P('ep', None, 'tp'), may hold values from -0.125 to 0.125
- w_up: bfloat16 [32, 2048, 6144], P('ep', None, 'tp'), may hold values from -0.125 to 0.125
- w_down: bfloat16 [32, 6144, 2048], P('ep', 'tp'), may hold values from -1.2757759 to 1.2757759
- routes: int32 [8192, 2], P('ep'), may hold values from 0 to 31, all different within a row; in each aligned block of 256 rows (0 to 255, 256 to 511, ...) at most 32 rows name the same one
- route_weights: float32 [8192, 2], P('ep'), may hold values from 0.1 to 1
- final_gain: bfloat16 [2048], P('tp'), may hold values from 0.099609375 to 1.8984375
Outputs:
- mixed_out: bfloat16 [8192, 2048], P('ep', 'tp')
The draws below stay inside these ranges and needn't reach their ends.
Inputs may be any that keep to these rules, and one draw needn't show every extreme that they name: `routes`: A token's 2 experts differ. Among the tokens of one index of ep (aligned blocks of 256 rows), no expert is named by more than 32 tokens, a bound that some block reaches.
All inputs are finite; a program needn't handle non-finite values.
Results may differ from the reference program's by a relative error of at most 0.017.
Values may be sent and summed in bfloat16 or wider, within the bound.
A program may use at most 64 MiB of HBM per device.

```python
import math
import jax
import jax.numpy as jnp
import numpy as np
from jax import lax

D = 2048
FF = 6144
TOPK = 2
TOK_DEV = 256
EXPERTS = 32
CAP = 32
TOKENS = 8192
N_EP = 32
N_TP = 16


def draw_tokens(key, part):
    first, second = jax.random.split(jax.random.fold_in(key, 11))
    scales = 10.0 ** jax.random.uniform(first, (TOKENS, 1), jnp.float32)
    columns = 10.0 ** (jnp.arange(D, dtype=jnp.float32) / (D - 1))
    base = jnp.clip(jax.random.normal(second, (TOKENS, D), jnp.float32), -4.0, 4.0)
    return (base * scales * columns[None, :]).astype(jnp.bfloat16)


def draw_w_down(key, part):
    first = jax.random.fold_in(jax.random.fold_in(key, 23), 0)
    columns = jnp.arange(D, dtype=jnp.float32) / (D - 1)
    scales = 10.0 ** columns
    base = jnp.clip(jax.random.normal(first, (EXPERTS, FF, D), jnp.float32), -4.0, 4.0)
    return (base * scales[None, None, :] * FF ** (-0.5)).astype(jnp.bfloat16)


def steps_of(stream_key, dims, pieces, smallest, largest):
    loudness, own = 1.0, jax.random.fold_in(stream_key, 6)
    for axis_at, blocks in pieces:
        draws = jnp.exp(jax.random.uniform(jax.random.fold_in(own, axis_at), (blocks,), jnp.float32, smallest / len(pieces), largest / len(pieces)))
        loudness = loudness * jnp.repeat(draws, dims[axis_at] // blocks).reshape([-1 if axis == axis_at else 1 for axis in range(len(dims))])
    return loudness


def deal_out(key, own, number, rows, count, top, limit, skew):
    sequence = jax.random.permutation(key, count)
    crowded, common = load_shares(count, rows * top, limit, skew, True), load_shares(count, rows * top, limit, skew, False)
    places = jnp.arange(count)

    def named(sizes, rotation):
        used = int((sizes > 0).sum())
        fixed = max(1, used // 4)
        shifted = fixed + (places - fixed + rotation * (used - fixed)) % max(1, count - fixed)
        return jnp.zeros((count,), jnp.int32).at[sequence[jnp.where(places < fixed, places, shifted)]].set(jnp.asarray(sizes, jnp.int32))

    sizes = jnp.where(number % 4 == 0, named(crowded, number // 4), named(common, number - number // 4 - 1))
    mixed = jax.random.permutation(jax.random.fold_in(own, 3), count)
    donor, sink = mixed[0:count // 2 * 2:2], mixed[1:count // 2 * 2:2]
    slack = jnp.minimum(sizes[donor] - 1, limit - sizes[sink]) // 2
    slack = jnp.where((donor == sequence[0]) | (sink == sequence[0]) | (sizes[sink] == 0), 0, jnp.maximum(slack, 0))
    shifted = jax.random.randint(jax.random.fold_in(own, 4), (count // 2,), 0, 1 << 20) % (slack + 1)
    sizes = sizes.at[donor].add(-shifted).at[sink].add(shifted)
    labels = jnp.searchsorted(jnp.cumsum(sizes), jnp.arange(rows * top), side="right").astype(jnp.int32)
    grid = labels.reshape(top, rows).T
    grid = grid[jax.random.permutation(jax.random.fold_in(own, 1), rows)]
    rotation = jax.random.randint(jax.random.fold_in(own, 2), (rows, 1), 0, top)
    return jnp.take_along_axis(grid, (jnp.arange(top)[None, :] + rotation) % top, axis=1)


def load_shares(count, total, limit, slope, full):
    portions = [(1 << 20) // math.isqrt(rank ** slope) + 1 for rank in range(1, count + 1)]
    largest = limit if full else min(limit, max(-(-total // count), total * portions[0] // sum(portions)))
    least = 1 if total - largest >= count - 1 else 0
    given, spare = [largest] + [least] * (count - 1), total - largest - least * (count - 1)
    while spare > 0:
        free = [i for i in range(1, count) if given[i] < largest] or [i for i in range(1, count) if given[i] < limit]
        mass, budget = sum([portions[i] for i in free]), spare
        for i in free:
            extra = min(limit - given[i], max(1, budget * portions[i] // mass), spare)
            given[i] = given[i] + extra
            spare = spare - extra
    return np.array(given)


def scatter_about(key, dims, spread, limit, pieces=(), kind=jnp.bfloat16):
    drawn = spread * jax.random.normal(key, dims, jnp.float32)
    if pieces:
        drawn = drawn * steps_of(key, dims, pieces, -0.22, 0.18)
    return jnp.clip(drawn, -limit, limit).astype(kind)


def setup_inputs(seed: int = 0) -> dict:
    streams_of = jax.random.split(jax.random.key(seed), 9)
    tokens = draw_tokens(jax.random.fold_in(streams_of[8], 71), 0)
    norm_gain = jnp.clip(1.0 + 0.18 * jax.random.normal(streams_of[1], (D,), jnp.float32), 0.099609375, 1.8984375).astype(jnp.bfloat16)
    w_gate = scatter_about(streams_of[2], (EXPERTS, D, FF), D ** -0.5, 0.125, ((0, 32), (2, 16)))
    w_up = scatter_about(streams_of[3], (EXPERTS, D, FF), D ** -0.5, 0.125, ((0, 32), (2, 16)))
    w_down = draw_w_down(jax.random.fold_in(streams_of[8], 71), 0)
    routes_keys = jax.random.split(jax.random.fold_in(streams_of[5], 1), TOKENS // TOK_DEV)
    routes_turns = jax.random.permutation(jax.random.fold_in(streams_of[5], 3), TOKENS // TOK_DEV)
    routes = jax.vmap(lambda own, number: deal_out(jax.random.fold_in(streams_of[5], 2), own, number, TOK_DEV, EXPERTS, TOPK, CAP, 2))(routes_keys, routes_turns).reshape((TOKENS, TOPK))
    route_weights = jnp.clip(0.1 + 0.9 * jax.random.uniform(streams_of[6], (TOKENS, TOPK), jnp.float32) ** steps_of(streams_of[6], (TOKENS, TOPK), ((0, 32),), -0.2, 0.2), 0.1, 1.0)
    final_gain = jnp.clip(1.0 + 0.18 * jax.random.normal(streams_of[7], (D,), jnp.float32), 0.099609375, 1.8984375).astype(jnp.bfloat16)
    return {"tokens": tokens, "norm_gain": norm_gain, "w_gate": w_gate, "w_up": w_up, "w_down": w_down, "routes": routes, "route_weights": route_weights, "final_gain": final_gain}


EPS = 1e-06

def reference(tokens, norm_gain, w_gate, w_up, w_down, routes, route_weights, final_gain):
    wide = tokens.astype(jnp.float32)
    scale = lax.rsqrt(lax.optimization_barrier(jnp.mean(wide * wide, axis=1, keepdims=True)) + EPS)
    normed = (wide * scale * norm_gain.astype(jnp.float32)[None, :]).astype(jnp.bfloat16)
    groups = routes.reshape(N_EP, TOK_DEV * TOPK)
    onehot = (groups[:, :, None] == jnp.arange(EXPERTS, dtype=jnp.int32)[None, None, :]).astype(jnp.int32)
    before = jnp.cumsum(onehot, axis=1) - onehot
    slot = lax.optimization_barrier(jnp.sum(before * onehot, axis=2)).astype(jnp.int32)
    source = jnp.broadcast_to(jnp.arange(N_EP, dtype=jnp.int32)[:, None], groups.shape)
    token_ids = jnp.repeat(jnp.arange(TOKENS, dtype=jnp.int32), TOPK).reshape(N_EP, TOK_DEV * TOPK)
    buffer = jnp.zeros((EXPERTS, N_EP, CAP, D), jnp.bfloat16)
    buffer = buffer.at[groups, source, slot].set(normed[token_ids])

    def one_expert(args):
        rows, gate_w, up_w, down_w = args
        rows = rows.reshape(N_EP * CAP, D).astype(jnp.float32)
        gate = jnp.dot(rows, gate_w.astype(jnp.float32), preferred_element_type=jnp.float32)
        up = jnp.dot(rows, up_w.astype(jnp.float32), preferred_element_type=jnp.float32)
        hidden = (jax.nn.silu(gate) * up).astype(jnp.bfloat16)
        blocks = hidden.reshape(N_EP * CAP, N_TP, FF // N_TP).astype(jnp.float32)
        down_blocks = down_w.reshape(N_TP, FF // N_TP, D).astype(jnp.float32)
        parts = jnp.einsum('rbf,bfd->brd', blocks, down_blocks).astype(jnp.bfloat16)
        return lax.optimization_barrier(jnp.sum(parts.astype(jnp.float32), axis=0)).astype(jnp.bfloat16)
    results = lax.map(one_expert, (buffer, w_gate, w_up, w_down))
    results = results.reshape(EXPERTS, N_EP, CAP, D)
    picked = results[groups, source, slot].reshape(TOKENS, TOPK, D)
    combined = jnp.einsum('tkd,tk->td', picked.astype(jnp.float32), route_weights)
    final_scale = lax.rsqrt(lax.optimization_barrier(jnp.mean(combined * combined, axis=1, keepdims=True)) + EPS)
    return (combined * final_scale * final_gain.astype(jnp.float32)[None, :]).astype(jnp.bfloat16)
```

```python
import functools

import jax
import jax.numpy as jnp
from jax import lax
from jax.experimental import pallas as pl
from jax.experimental.pallas import tpu as pltpu
from jax.sharding import PartitionSpec as P

EPS = 1e-06
LANES = 128
MESH = pl.DeviceIdType.MESH
BF, F32 = jnp.bfloat16, jnp.float32

ORDERS = (
    (("x", 0), ("y", 0), ("x", 1), ("y", 1)),
    (("y", 0), ("x", 1), ("y", 1), ("x", 0)),
    (("x", 1), ("y", 1), ("x", 0), ("y", 0)),
    (("y", 1), ("x", 0), ("y", 0), ("x", 1)),
)
STAGGER = 3


def block_index(quarter, y, x):
    place = {}
    index = 0
    seen = {"x": 0, "y": 0}
    for bit, (axis, parity) in enumerate(ORDERS[quarter]):
        at = x if axis == "x" else y
        if seen[axis] == 0:
            place[axis] = (at + parity) % 4
            index = index + (place[axis] % 2) * 2**bit
        else:
            index = index + (place[axis] // 2) * 2**bit
        seen[axis] += 1
    return index


def partner(axis, parity, y, x):
    at = x if axis == "x" else y
    step = 1 - 2 * ((at + parity) % 2)
    other = (at + step + 4) % 4
    return y * 4 + other if axis == "x" else other * 4 + x


def distances(chips):
    out = [0]
    for d in range(1, chips // 2 + 1):
        out.append(d)
        if d != chips - d:
            out.append(-d)
    return out


def body(
    chips,
    tok_ref,
    gain_ref,
    routes_ref,
    rw_ref,
    fg_ref,
    wg_hbm,
    wu_hbm,
    wd_hbm,
    out_ref,
    w1,
    wd,
    outbox,
    gather,
    normed,
    parts,
    in0,
    in1,
    in2,
    in3,
    done,
    returned,
    gains,
    squares,
    w_sem,
    disp_send,
    disp_recv,
    ag_send,
    ag_recv,
    rs_send,
    rs_recv,
    ret_send,
    ret_recv,
    gain_send,
    gain_recv,
    sq_send,
    sq_recv,
):
    inbound = (in0, in1, in2, in3)
    ep, tp = lax.axis_index("ep"), lax.axis_index("tp")
    z, core = ep // 2, ep % 2
    y, x = tp // 4, tp % 4
    tokens = tok_ref.shape[0]
    experts, cap = outbox.shape[0], outbox.shape[1]
    items = chips
    rounds = items // 4
    rows = 2 * cap
    width = 16 * LANES
    hidden_units = wd.shape[0]
    dz = distances(chips)

    loads = (
        pltpu.make_async_copy(wg_hbm.at[0], w1.at[:, pl.ds(0, hidden_units)], w_sem.at[0]),
        pltpu.make_async_copy(wu_hbm.at[0], w1.at[:, pl.ds(hidden_units, hidden_units)], w_sem.at[1]),
        pltpu.make_async_copy(wd_hbm.at[0], wd, w_sem.at[2]),
    )
    for load in loads:
        load.start()

    def ahead(item, dc):
        return ((z + dz[item] + chips) % chips) * 2 + (core + dc) % 2

    def behind(item, dc):
        return ((z - dz[item] + chips) % chips) * 2 + (core + dc) % 2

    barrier = pltpu.get_barrier_semaphore()
    far = [(item, dc) for item in range(items) for dc in range(2) if (item, dc) != (0, 0)]
    for item, dc in reversed(far):
        pl.semaphore_signal(barrier, inc=1, device_id=(ahead(item, dc), tp), device_id_type=MESH)
    for off in range(1, 16):
        pl.semaphore_signal(barrier, inc=1, device_id=(ep, (tp + off) % 16), device_id_type=MESH)

    r0 = jnp.broadcast_to(routes_ref[:, 0:1], (tokens, LANES))
    r1 = jnp.broadcast_to(routes_ref[:, 1:2], (tokens, LANES))
    lane = lax.broadcasted_iota(jnp.int32, (tokens, LANES), 1)
    hit0 = jnp.where(r0 == lane, 1.0, 0.0).astype(F32)
    hit1 = jnp.where(r1 == lane, 1.0, 0.0).astype(F32)
    below = jnp.where(
        lax.broadcasted_iota(jnp.int32, (tokens, tokens), 0) > lax.broadcasted_iota(jnp.int32, (tokens, tokens), 1),
        1.0,
        0.0,
    ).astype(BF)
    before = jnp.dot(below, (hit0 + hit1).astype(BF), preferred_element_type=F32)
    target0 = jnp.sum(hit0 * (before + lane.astype(F32) * cap), axis=1, keepdims=True)
    target1 = jnp.sum(hit1 * (before + lane.astype(F32) * cap), axis=1, keepdims=True)
    across0 = jnp.transpose(jnp.broadcast_to(target0, (tokens, LANES)))[0:1, :]
    across1 = jnp.transpose(jnp.broadcast_to(target1, (tokens, LANES)))[0:1, :]
    piece = 256
    for start in range(0, experts * cap, piece):
        slot = (lax.broadcasted_iota(jnp.int32, (piece, tokens), 0) + start).astype(F32)
        pick = jnp.where((slot == across0) | (slot == across1), 1.0, 0.0).astype(BF)
        picked = jnp.dot(pick, tok_ref[...], preferred_element_type=F32).astype(BF)
        outbox[pl.ds(start // cap, piece // cap)] = picked.reshape(piece // cap, cap, LANES)
    gains[pl.ds(tp, 1)] = gain_ref[...].astype(F32).reshape(1, 1, LANES)

    pl.semaphore_wait(barrier, len(far) + 15)

    mine = [block_index(q, y, x) for q in range(4)]
    gather[0, pl.ds(mine[0], 1), pl.ds(0, cap)] = outbox[pl.ds(ep, 1)]

    def dispatch(item, dc):
        return pltpu.make_async_remote_copy(
            src_ref=outbox.at[ahead(item, dc)],
            dst_ref=gather.at[item, mine[item % 4], pl.ds(dc * cap, cap)],
            send_sem=disp_send.at[item, dc],
            recv_sem=disp_recv.at[item, dc],
            device_id=(ahead(item, dc), tp),
            device_id_type=MESH,
        )

    for item, dc in far:
        dispatch(item, dc).start()

    def small(buffer, sends, recvs, off):
        return pltpu.make_async_remote_copy(
            src_ref=buffer.at[tp],
            dst_ref=buffer.at[tp],
            send_sem=sends.at[off],
            recv_sem=recvs.at[off],
            device_id=(ep, (tp + off) % 16),
            device_id_type=MESH,
        )

    for off in range(1, 16):
        small(gains, gain_send, gain_recv, off).start()

    def gather_copy(item, stage):
        axis, parity = ORDERS[item % 4][stage]
        group = pl.ds((mine[item % 4] // 2**stage) * 2**stage, 2**stage)
        return pltpu.make_async_remote_copy(
            src_ref=gather.at[item, group],
            dst_ref=gather.at[item, group],
            send_sem=ag_send.at[item, stage],
            recv_sem=ag_recv.at[item, stage],
            device_id=(ep, partner(axis, parity, y, x)),
            device_id_type=MESH,
        )

    def scatter_copy(item, stage):
        bit = 3 - stage
        axis, parity = ORDERS[item % 4][bit]
        index = mine[item % 4]
        base = (index // 2 ** (bit + 1)) * 2 ** (bit + 1)
        sent = base + (1 - (index // 2**bit) % 2) * 2**bit
        return pltpu.make_async_remote_copy(
            src_ref=parts.at[item, pl.ds(sent, 2**bit)],
            dst_ref=inbound[stage].at[item],
            send_sem=rs_send.at[item, stage],
            recv_sem=rs_recv.at[item, stage],
            device_id=(ep, partner(axis, parity, y, x)),
            device_id_type=MESH,
        )

    def give_back(item, dc):
        return pltpu.make_async_remote_copy(
            src_ref=done.at[item, pl.ds(dc * cap, cap)],
            dst_ref=returned.at[ep],
            send_sem=ret_send.at[item, dc],
            recv_sem=ret_recv.at[item, dc],
            device_id=(behind(item, dc), tp),
            device_id_type=MESH,
        )

    def gather_stage(k, stage):
        for q in range(4):
            item = 4 * k + q
            if stage == 0:
                for dc in range(2):
                    if (item, dc) != (0, 0):
                        dispatch(item, dc).wait_recv()
            else:
                gather_copy(item, stage - 1).wait_recv()
            gather_copy(item, stage).start()

    def experts_stage(k):
        if k == 0:
            for off in range(1, 16):
                small(gains, gain_send, gain_recv, off).wait_recv()
            for load in loads:
                load.wait()
        for q in range(4):
            item = 4 * k + q
            gather_copy(item, 3).wait_recv()
            total = jnp.zeros((rows, LANES), F32)
            for t in range(16):
                row = gather[item, block_index(q, t // 4, t % 4)].astype(F32)
                total = total + row * row
            scale = lax.rsqrt(jnp.sum(total, axis=1, keepdims=True) / width + EPS)
            scale = jnp.broadcast_to(scale, (rows, LANES))
            for t in range(16):
                row = gather[item, block_index(q, t // 4, t % 4)].astype(F32)
                normed[pl.ds(q * rows, rows), pl.ds(t * LANES, LANES)] = (row * scale * gains[t]).astype(BF)
        both = jnp.dot(normed[...], w1[...], preferred_element_type=F32)
        gate, up = both[:, :hidden_units], both[:, hidden_units:]
        hidden = (gate / (1.0 + jnp.exp(-gate)) * up).astype(BF)
        for pair in range(8):
            part = jnp.dot(hidden, wd[:, pl.ds(pair * 256, 256)], preferred_element_type=F32).astype(BF)
            for q in range(4):
                for t in (2 * pair, 2 * pair + 1):
                    parts[4 * k + q, block_index(q, t // 4, t % 4)] = part[
                        q * rows : (q + 1) * rows, (t % 2) * LANES : (t % 2 + 1) * LANES
                    ]
        for q in range(4):
            scatter_copy(4 * k + q, 0).start()

    def scatter_stage(k, stage):
        for q in range(4):
            item = 4 * k + q
            scatter_copy(item, stage - 1).wait_recv()
            bit = 4 - stage
            kept = pl.ds((mine[q] // 2**bit) * 2**bit, 2**bit)
            added = (parts[item, kept].astype(F32) + inbound[stage - 1][item].astype(F32)).astype(BF)
            if stage < 4:
                parts[item, kept] = added
            else:
                done[item] = added[0]
        for q in range(4):
            item = 4 * k + q
            if stage < 4:
                scatter_copy(item, stage).start()
            else:
                for dc in range(2):
                    if (item, dc) == (0, 0):
                        returned[pl.ds(ep, 1)] = done[0, pl.ds(0, cap)].reshape(1, cap, LANES)
                    else:
                        give_back(item, dc).start()

    schedule = []
    for k in range(rounds):
        for s in range(4):
            schedule.append((s + STAGGER * k, k, functools.partial(gather_stage, k, s)))
        schedule.append((4 + STAGGER * k, k, functools.partial(experts_stage, k)))
        for s in range(1, 5):
            schedule.append((4 + s + STAGGER * k, k, functools.partial(scatter_stage, k, s)))
    for _, _, run in sorted(schedule, key=lambda entry: entry[:2]):
        run()

    for item, dc in far:
        give_back(item, dc).wait_recv()
    slot = lax.broadcasted_iota(jnp.int32, (tokens, experts * cap), 1).astype(F32)
    mix = jnp.where(slot == target0, rw_ref[:, 0:1], 0.0) + jnp.where(slot == target1, rw_ref[:, 1:2], 0.0)
    high = mix.astype(BF)
    low = (mix - high.astype(F32)).astype(BF)
    results = returned[...].reshape(experts * cap, LANES)
    combined = jnp.dot(high, results, preferred_element_type=F32) + jnp.dot(low, results, preferred_element_type=F32)

    squares[pl.ds(tp, 1)] = jnp.sum(jnp.transpose(combined * combined), axis=0, keepdims=True).reshape(1, 1, tokens)
    for off in range(1, 16):
        small(squares, sq_send, sq_recv, off).start()
    for off in range(1, 16):
        small(squares, sq_send, sq_recv, off).wait_recv()
    total = squares[0]
    for t in range(1, 16):
        total = total + squares[t]
    final = lax.rsqrt(total / width + EPS)
    final = jnp.transpose(jnp.broadcast_to(final, (LANES, tokens)))
    out_ref[...] = (combined * final * fg_ref[...].astype(F32)).astype(BF)

    for item, dc in far:
        dispatch(item, dc).wait_send()
        give_back(item, dc).wait_send()
    for off in range(1, 16):
        small(gains, gain_send, gain_recv, off).wait_send()
        small(squares, sq_send, sq_recv, off).wait_send()
    for item in range(items):
        for stage in range(4):
            gather_copy(item, stage).wait_send()
            scatter_copy(item, stage).wait_send()


def local(tokens, norm_gain, w_gate, w_up, w_down, routes, route_weights, final_gain):
    experts = lax.axis_size("ep")
    chips = experts // 2
    tok_rows, share = tokens.shape
    cap = 2 * tok_rows * routes.shape[1] // experts
    hidden_units = w_gate.shape[2]
    rows = 2 * cap
    vmem = pl.BlockSpec(memory_space=pltpu.VMEM)
    hbm = pl.BlockSpec(memory_space=pl.ANY)
    dma = pltpu.SemaphoreType.DMA
    return pl.pallas_call(
        functools.partial(body, chips),
        out_shape=jax.ShapeDtypeStruct((tok_rows, share), BF),
        in_specs=[vmem] * 5 + [hbm] * 3,
        out_specs=vmem,
        scratch_shapes=[
            pltpu.VMEM((16 * share, 2 * hidden_units), BF),
            pltpu.VMEM((hidden_units, 16 * share), BF),
            pltpu.VMEM((experts, cap, share), BF),
            pltpu.VMEM((chips, 16, rows, share), BF),
            pltpu.VMEM((4 * rows, 16 * share), BF),
            pltpu.VMEM((chips, 16, rows, share), BF),
            pltpu.VMEM((chips, 8, rows, share), BF),
            pltpu.VMEM((chips, 4, rows, share), BF),
            pltpu.VMEM((chips, 2, rows, share), BF),
            pltpu.VMEM((chips, 1, rows, share), BF),
            pltpu.VMEM((chips, rows, share), BF),
            pltpu.VMEM((experts, cap, share), BF),
            pltpu.VMEM((16, 1, share), F32),
            pltpu.VMEM((16, 1, tok_rows), F32),
            dma((3,)),
            dma((chips, 2)),
            dma((chips, 2)),
            dma((chips, 4)),
            dma((chips, 4)),
            dma((chips, 4)),
            dma((chips, 4)),
            dma((chips, 2)),
            dma((chips, 2)),
            dma((16,)),
            dma((16,)),
            dma((16,)),
            dma((16,)),
        ],
        compiler_params=pltpu.CompilerParams(collective_id=0, has_side_effects=True),
    )(
        tokens,
        norm_gain.reshape(1, -1),
        routes,
        route_weights,
        final_gain.reshape(1, -1),
        w_gate,
        w_up,
        w_down,
    )


def solution(mesh):
    in_specs = (
        P("ep", "tp"),
        P("tp"),
        P("ep", None, "tp"),
        P("ep", None, "tp"),
        P("ep", "tp", None),
        P("ep", None),
        P("ep", None),
        P("tp"),
    )
    out_specs = P("ep", "tp")
    return jax.shard_map(local, mesh=mesh, in_specs=in_specs, out_specs=out_specs, check_vma=False)
```

```python
import functools

import jax
import jax.numpy as jnp
from jax import lax
from jax.experimental import pallas as pl
from jax.experimental.pallas import tpu as pltpu
from jax.sharding import PartitionSpec as P

EPS = 1e-06
LANES = 128
MESH = pl.DeviceIdType.MESH
BF, F32 = jnp.bfloat16, jnp.float32

ORDERS = (
    (("x", 0), ("y", 0), ("x", 1), ("y", 1)),
    (("y", 0), ("x", 1), ("y", 1), ("x", 0)),
    (("x", 1), ("y", 1), ("x", 0), ("y", 0)),
    (("y", 1), ("x", 0), ("y", 0), ("x", 1)),
)
ORDER = (
    (0, 0), (1, 0), (0, 1), (1, 1), (0, 2), (2, 0), (3, 0), (1, 2), (2, 1), (3, 1), (0, 3), (2, 2),
    (3, 2), (1, 3), (3, 3), (2, 3), (1, 4), (3, 4), (2, 4), (0, 4), (3, 5), (2, 5), (1, 5), (3, 6),
    (0, 5), (2, 6), (1, 6), (3, 7), (0, 6), (2, 7), (1, 7), (3, 8), (0, 7), (2, 8), (1, 8), (0, 8),
)


def block_index(quarter, y, x):
    place = {}
    index = 0
    seen = {"x": 0, "y": 0}
    for bit, (axis, parity) in enumerate(ORDERS[quarter]):
        at = x if axis == "x" else y
        if seen[axis] == 0:
            place[axis] = (at + parity) % 4
            index = index + (place[axis] % 2) * 2**bit
        else:
            index = index + (place[axis] // 2) * 2**bit
        seen[axis] += 1
    return index


def partner(axis, parity, y, x):
    at = x if axis == "x" else y
    step = 1 - 2 * ((at + parity) % 2)
    other = (at + step + 4) % 4
    return y * 4 + other if axis == "x" else other * 4 + x


def distances(chips):
    out = [0]
    for d in range(1, chips // 2 + 1):
        out.append(d)
        if d != chips - d:
            out.append(-d)
    return out


def body(
    chips,
    tok_ref,
    gain_ref,
    routes_ref,
    rw_ref,
    fg_ref,
    wg_hbm,
    wu_hbm,
    wd_hbm,
    out_ref,
    w1,
    wd,
    outbox,
    gather,
    normed,
    parts,
    in0,
    in1,
    in2,
    in3,
    done,
    returned,
    gains,
    squares,
    w_sem,
    disp_send,
    disp_recv,
    ag_send,
    ag_recv,
    rs_send,
    rs_recv,
    ret_send,
    ret_recv,
    gain_send,
    gain_recv,
    sq_send,
    sq_recv,
    high,
    low,
    entered,
):
    inbound = (in0, in1, in2, in3)
    ep, tp = lax.axis_index("ep"), lax.axis_index("tp")
    z, core = ep // 2, ep % 2
    y, x = tp // 4, tp % 4
    tokens = tok_ref.shape[0]
    experts, cap = outbox.shape[0], outbox.shape[1]
    items = chips
    rounds = items // 4
    rows = 2 * cap
    width = 16 * LANES
    hidden_units = wd.shape[0]
    dz = distances(chips)

    loads = (
        pltpu.make_async_copy(wg_hbm.at[0], w1.at[:, pl.ds(0, hidden_units)], w_sem.at[0]),
        pltpu.make_async_copy(wu_hbm.at[0], w1.at[:, pl.ds(hidden_units, hidden_units)], w_sem.at[1]),
        pltpu.make_async_copy(wd_hbm.at[0], wd, w_sem.at[2]),
    )
    for load in loads:
        load.start()

    def ahead(item, dc):
        return ((z + dz[item] + chips) % chips) * 2 + (core + dc) % 2

    def behind(item, dc):
        return ((z - dz[item] + chips) % chips) * 2 + (core + dc) % 2

    barrier = pltpu.get_barrier_semaphore()

    def along(step, dc):
        return ((z + step + chips) % chips) * 2 + (core + dc) % 2

    near = [(along(step, dc), tp) for step in (-2, -1, 0, 1, 2) for dc in range(2) if (step, dc) != (0, 0)]
    near += [(ep, partner(axis, parity, y, x)) for axis, parity in ORDERS[0]]
    for device in near:
        pl.semaphore_signal(barrier, inc=1, device_id=device, device_id_type=MESH)
    far = [(item, dc) for item in range(items) for dc in range(2) if (item, dc) != (0, 0)]

    prep = jax.named_scope("prep")
    prep.__enter__()
    expert = lax.broadcasted_iota(jnp.int32, (experts, tokens), 0)
    hit0 = jnp.where(routes_ref[0:1, :] == expert, 1.0, 0.0).astype(F32)
    hit1 = jnp.where(routes_ref[1:2, :] == expert, 1.0, 0.0).astype(F32)
    above = jnp.where(
        lax.broadcasted_iota(jnp.int32, (tokens, tokens), 0) < lax.broadcasted_iota(jnp.int32, (tokens, tokens), 1),
        1.0,
        0.0,
    ).astype(BF)
    before = jnp.dot((hit0 + hit1).astype(BF), above, preferred_element_type=F32)
    base = before + expert.astype(F32) * cap
    target0 = jnp.sum(hit0 * base, axis=0, keepdims=True)
    target1 = jnp.sum(hit1 * base, axis=0, keepdims=True)
    piece = 256
    for start in range(0, experts * cap, piece):
        slot = (lax.broadcasted_iota(jnp.int32, (piece, tokens), 0) + start).astype(F32)
        pick = jnp.where((slot == target0) | (slot == target1), 1.0, 0.0).astype(BF)
        picked = jnp.dot(pick, tok_ref[...], preferred_element_type=F32).astype(BF)
        outbox[pl.ds(start // cap, piece // cap)] = picked.reshape(piece // cap, cap, LANES)
    mine = [block_index(q, y, x) for q in range(4)]
    gains[pl.ds(mine[0], 1)] = gain_ref[...].astype(F32).reshape(1, 1, LANES)
    prep.__exit__(None, None, None)

    with jax.named_scope("barrier"):
        pl.semaphore_wait(barrier, len(near))

    gather[0, pl.ds(mine[0], 1), pl.ds(0, cap)] = outbox[pl.ds(ep, 1)]

    def dispatch(item, dc):
        return pltpu.make_async_remote_copy(
            src_ref=outbox.at[ahead(item, dc)],
            dst_ref=gather.at[item, mine[item % 4], pl.ds(dc * cap, cap)],
            send_sem=disp_send,
            recv_sem=disp_recv.at[item],
            device_id=(ahead(item, dc), tp),
            device_id_type=MESH,
        )

    def dispatch_round(k):
        for item, dc in far:
            if item // 4 == k:
                dispatch(item, dc).start()

    def tell(level):
        for way, step in enumerate((-(2**level), 2**level)):
            pl.semaphore_signal(
                entered.at[level - 1, way], inc=1, device_id=(along(step, 0), tp), device_id_type=MESH
            )

    def hear(level):
        for way in range(2):
            pl.semaphore_wait(entered.at[level - 1, way], 1)

    dispatch_round(0)
    tell(1)

    with jax.named_scope("weights"):
        line = lax.broadcasted_iota(jnp.int32, (LANES, tokens), 0)
        stacked = jnp.where(line == 0, target0, jnp.where(line == 1, target1, 0.0))
        stacked = jnp.where(line == 2, rw_ref[0:1, :], jnp.where(line == 3, rw_ref[1:2, :], stacked))
        columns = jnp.transpose(stacked)
        slot = lax.broadcasted_iota(jnp.int32, (tokens, experts * cap), 1).astype(F32)
        mix = jnp.where(slot == columns[:, 0:1], columns[:, 2:3], 0.0)
        mix = mix + jnp.where(slot == columns[:, 1:2], columns[:, 3:4], 0.0)
        upper = mix.astype(BF)
        high[...] = upper
        low[...] = (mix - upper.astype(F32)).astype(BF)
    with jax.named_scope("hear1"):
        hear(1)
    tell(2)

    dispatch_round(1)

    def later_rounds():
        hear(2)
        for k in range(2, rounds):
            dispatch_round(k)

    def all_of(ref, sem):
        pltpu.make_async_copy(ref, ref, sem).wait()

    def square_copy(off):
        return pltpu.make_async_remote_copy(
            src_ref=squares.at[tp],
            dst_ref=squares.at[tp],
            send_sem=sq_send,
            recv_sem=sq_recv,
            device_id=(ep, (tp + off) % 16),
            device_id_type=MESH,
        )

    def gain_copy(stage):
        axis, parity = ORDERS[0][stage]
        group = pl.ds((mine[0] // 2**stage) * 2**stage, 2**stage)
        return pltpu.make_async_remote_copy(
            src_ref=gains.at[group],
            dst_ref=gains.at[group],
            send_sem=gain_send,
            recv_sem=gain_recv.at[stage],
            device_id=(ep, partner(axis, parity, y, x)),
            device_id_type=MESH,
        )

    def gather_copy(item, stage):
        axis, parity = ORDERS[item % 4][stage]
        group = pl.ds((mine[item % 4] // 2**stage) * 2**stage, 2**stage)
        return pltpu.make_async_remote_copy(
            src_ref=gather.at[item, group],
            dst_ref=gather.at[item, group],
            send_sem=ag_send,
            recv_sem=ag_recv.at[item, stage],
            device_id=(ep, partner(axis, parity, y, x)),
            device_id_type=MESH,
        )

    def scatter_copy(item, stage):
        bit = 3 - stage
        axis, parity = ORDERS[item % 4][bit]
        index = mine[item % 4]
        base = (index // 2 ** (bit + 1)) * 2 ** (bit + 1)
        sent = base + (1 - (index // 2**bit) % 2) * 2**bit
        return pltpu.make_async_remote_copy(
            src_ref=parts.at[item, pl.ds(sent, 2**bit)],
            dst_ref=inbound[stage].at[item],
            send_sem=rs_send,
            recv_sem=rs_recv.at[item, stage],
            device_id=(ep, partner(axis, parity, y, x)),
            device_id_type=MESH,
        )

    def give_back(item, dc):
        return pltpu.make_async_remote_copy(
            src_ref=done.at[item, pl.ds(dc * cap, cap)],
            dst_ref=returned.at[ep],
            send_sem=ret_send,
            recv_sem=ret_recv,
            device_id=(behind(item, dc), tp),
            device_id_type=MESH,
        )

    def gather_stage(k, stage):
        for q in range(4):
            item = 4 * k + q
            if stage == 0:
                filled = pl.ds(cap, cap) if item == 0 else pl.ds(0, rows)
                all_of(gather.at[item, 0, filled], disp_recv.at[item])
            else:
                gather_copy(item, stage - 1).wait_recv()
            gather_copy(item, stage).start()
        if k == 0:
            if stage > 0:
                gain_copy(stage - 1).wait_recv()
            gain_copy(stage).start()

    first = [k for k, stage in ORDER if stage == 4][0]

    def experts_stage(k):
        for q in range(4):
            with jax.named_scope("mwait%d%d" % (k, q)):
                gather_copy(4 * k + q, 3).wait_recv()
        if k == first:
            gain_copy(3).wait_recv()
            for load in loads:
                load.wait()
        for q in range(4):
            item = 4 * k + q
            total = jnp.zeros((rows, LANES), F32)
            for t in range(16):
                row = gather[item, block_index(q, t // 4, t % 4)].astype(F32)
                total = total + row * row
            scale = lax.rsqrt(jnp.sum(total, axis=1, keepdims=True) / width + EPS)
            scale = jnp.broadcast_to(scale, (rows, LANES))
            for t in range(16):
                row = gather[item, block_index(q, t // 4, t % 4)].astype(F32)
                normed[pl.ds(q * rows, rows), pl.ds(t * LANES, LANES)] = (row * scale * gains[block_index(0, t // 4, t % 4)]).astype(BF)
        both = jnp.dot(normed[...], w1[...], preferred_element_type=F32)
        gate, up = both[:, :hidden_units], both[:, hidden_units:]
        hidden = (gate / (1.0 + jnp.exp(-gate)) * up).astype(BF)
        for pair in range(8):
            part = jnp.dot(hidden, wd[:, pl.ds(pair * 256, 256)], preferred_element_type=F32).astype(BF)
            for q in range(4):
                for t in (2 * pair, 2 * pair + 1):
                    parts[4 * k + q, block_index(q, t // 4, t % 4)] = part[
                        q * rows : (q + 1) * rows, (t % 2) * LANES : (t % 2 + 1) * LANES
                    ]
        for q in range(4):
            scatter_copy(4 * k + q, 0).start()

    def scatter_stage(k, stage):
        for q in range(4):
            item = 4 * k + q
            scatter_copy(item, stage - 1).wait_recv()
            bit = 4 - stage
            kept = pl.ds((mine[q] // 2**bit) * 2**bit, 2**bit)
            added = (parts[item, kept].astype(F32) + inbound[stage - 1][item].astype(F32)).astype(BF)
            if stage < 4:
                parts[item, kept] = added
            else:
                done[item] = added[0]
        for q in range(4):
            item = 4 * k + q
            if stage < 4:
                scatter_copy(item, stage).start()
            else:
                for dc in range(2):
                    if (item, dc) == (0, 0):
                        returned[pl.ds(ep, 1)] = done[0, pl.ds(0, cap)].reshape(1, cap, LANES)
                    else:
                        give_back(item, dc).start()

    for k, stage in ORDER:
        with jax.named_scope("r%d_s%d" % (k, stage)):
            if stage < 4:
                gather_stage(k, stage)
            elif stage == 4:
                experts_stage(k)
            else:
                scatter_stage(k, stage - 4)
        if (k, stage) == (0, 0):
            with jax.named_scope("later"):
                later_rounds()

    all_of(outbox.at[pl.ds(0, experts - 1)], disp_send)
    all_of(gains.at[pl.ds(0, 15)], gain_send)
    all_of(gather.at[:, pl.ds(0, 15)], ag_send)
    all_of(parts.at[:, pl.ds(0, 15)], rs_send)
    with jax.named_scope("retwait"):
        all_of(returned.at[pl.ds(0, experts - 1)], ret_recv)
    with jax.named_scope("combine"):
        results = returned[...].reshape(experts * cap, LANES)
        combined = jnp.dot(high[...], results, preferred_element_type=F32)
        combined = combined + jnp.dot(low[...], results, preferred_element_type=F32)
        square = jnp.sum(jnp.transpose(combined * combined), axis=0, keepdims=True)
        squares[pl.ds(tp, 1)] = square.reshape(1, 1, tokens)
        for off in range(1, 16):
            square_copy(off).start()
    all_of(outbox.at[pl.ds(0, experts - 1)], ret_send)
    with jax.named_scope("sqwait"):
        all_of(squares.at[pl.ds(0, 15)], sq_recv)
    total = squares[0]
    for t in range(1, 16):
        total = total + squares[t]
    final = lax.rsqrt(total / width + EPS)
    final = jnp.transpose(jnp.broadcast_to(final, (LANES, tokens)))
    out_ref[...] = (combined * final * fg_ref[...].astype(F32)).astype(BF)

    all_of(squares.at[pl.ds(0, 15)], sq_send)


def local(tokens, norm_gain, w_gate, w_up, w_down, routes, route_weights, final_gain):
    experts = lax.axis_size("ep")
    chips = experts // 2
    tok_rows, share = tokens.shape
    cap = 2 * tok_rows * routes.shape[1] // experts
    hidden_units = w_gate.shape[2]
    rows = 2 * cap
    vmem = pl.BlockSpec(memory_space=pltpu.VMEM)
    hbm = pl.BlockSpec(memory_space=pl.ANY)
    dma = pltpu.SemaphoreType.DMA
    return pl.pallas_call(
        functools.partial(body, chips),
        out_shape=jax.ShapeDtypeStruct((tok_rows, share), BF),
        in_specs=[vmem] * 5 + [hbm] * 3,
        out_specs=vmem,
        scratch_shapes=[
            pltpu.VMEM((16 * share, 2 * hidden_units), BF),
            pltpu.VMEM((hidden_units, 16 * share), BF),
            pltpu.VMEM((experts, cap, share), BF),
            pltpu.VMEM((chips, 16, rows, share), BF),
            pltpu.VMEM((4 * rows, 16 * share), BF),
            pltpu.VMEM((chips, 16, rows, share), BF),
            pltpu.VMEM((chips, 8, rows, share), BF),
            pltpu.VMEM((chips, 4, rows, share), BF),
            pltpu.VMEM((chips, 2, rows, share), BF),
            pltpu.VMEM((chips, 1, rows, share), BF),
            pltpu.VMEM((chips, rows, share), BF),
            pltpu.VMEM((experts, cap, share), BF),
            pltpu.VMEM((16, 1, share), F32),
            pltpu.VMEM((16, 1, tok_rows), F32),
            dma((3,)),
            dma,
            dma((chips,)),
            dma,
            dma((chips, 4)),
            dma,
            dma((chips, 4)),
            dma,
            dma,
            dma,
            dma((4,)),
            dma,
            dma,
            pltpu.VMEM((tok_rows, experts * cap), BF),
            pltpu.VMEM((tok_rows, experts * cap), BF),
            pltpu.SemaphoreType.REGULAR((2, 2)),
        ],
        compiler_params=pltpu.CompilerParams(collective_id=0, has_side_effects=True),
    )(
        tokens,
        norm_gain.reshape(1, -1),
        routes.T,
        route_weights.T,
        final_gain.reshape(1, -1),
        w_gate,
        w_up,
        w_down,
    )


def solution(mesh):
    in_specs = (
        P("ep", "tp"),
        P("tp"),
        P("ep", None, "tp"),
        P("ep", None, "tp"),
        P("ep", "tp", None),
        P("ep", None),
        P("ep", None),
        P("tp"),
    )
    out_specs = P("ep", "tp")
    return jax.shard_map(local, mesh=mesh, in_specs=in_specs, out_specs=out_specs, check_vma=False)
```

```python
import functools

import jax
import jax.numpy as jnp
from jax import lax
from jax.experimental import pallas as pl
from jax.experimental.pallas import tpu as pltpu
from jax.sharding import PartitionSpec as P

EPS = 1e-06
LANES = 128
MESH = pl.DeviceIdType.MESH
BF, F32 = jnp.bfloat16, jnp.float32

ORDERS = (
    (("x", 0), ("y", 0), ("x", 1), ("y", 1)),
    (("y", 0), ("x", 1), ("y", 1), ("x", 0)),
    (("x", 1), ("y", 1), ("x", 0), ("y", 0)),
    (("y", 1), ("x", 0), ("y", 0), ("x", 1)),
)
ORDER = (
    (0, 0), (1, 0), (0, 1), (1, 1), (0, 2), (3, 0), (2, 0), (0, 3), (3, 1), (2, 1), (1, 2), (3, 2),
    (2, 2), (1, 3), (3, 3), (2, 3), (0, 4), (3, 4), (2, 4), (3, 5), (1, 4), (3, 6), (2, 5), (1, 5),
    (3, 7), (2, 6), (0, 5), (1, 6), (3, 8), (2, 7), (0, 6), (1, 7), (2, 8), (0, 7), (1, 8), (0, 8),
)
SOURCES = 2


def block_index(quarter, y, x):
    place = {}
    index = 0
    seen = {"x": 0, "y": 0}
    for bit, (axis, parity) in enumerate(ORDERS[quarter]):
        at = x if axis == "x" else y
        if seen[axis] == 0:
            place[axis] = (at + parity) % 4
            index = index + (place[axis] % 2) * 2**bit
        else:
            index = index + (place[axis] // 2) * 2**bit
        seen[axis] += 1
    return index


def partner(axis, parity, y, x):
    at = x if axis == "x" else y
    step = 1 - 2 * ((at + parity) % 2)
    other = (at + step + 4) % 4
    return (y, other) if axis == "x" else (other, x)


def handed_on(index, bit):
    return (index // 2 ** (bit + 1)) * 2 ** (bit + 1) + (1 - (index // 2**bit) % 2) * 2**bit


def landing(stage, step):
    return 2 ** (3 - stage) - (2 ** (4 - step))


def distances(chips):
    out = [0]
    for d in range(1, chips // 2 + 1):
        out.append(d)
        if d != chips - d:
            out.append(-d)
    return out


def body(
    chips,
    tok_hbm,
    gain_hbm,
    routes_hbm,
    rw_hbm,
    fg_hbm,
    wg_hbm,
    wu_hbm,
    wd_hbm,
    out_ref,
    w1,
    wd,
    outbox,
    gather,
    normed,
    parts,
    in0,
    in1,
    in2,
    in3,
    done,
    returned,
    gains,
    squares,
    w_sem,
    disp_send,
    disp_recv,
    ag_send,
    ag_recv,
    rs_send,
    rs_recv,
    ret_send,
    ret_recv,
    gain_send,
    gain_recv,
    sq_send,
    sq_recv,
    high,
    low,
    entered,
    tok_ref,
    gain_ref,
    routes_ref,
    rw_ref,
    fg_ref,
    op_sem,
):
    inbound = (in0, in1, in2, in3)
    ep, tp = lax.axis_index("ep"), lax.axis_index("tp")
    z, core = ep // 2, ep % 2
    y, x = tp // 4, tp % 4
    tokens = tok_ref.shape[0]
    experts, cap = outbox.shape[0], outbox.shape[1]
    items = experts // SOURCES
    rounds = items // 4
    rows = SOURCES * cap
    width = 16 * LANES
    hidden_units = wd.shape[0]
    dz = distances(chips)

    def ahead(n):
        return ((z + dz[n // 2] + chips) % chips) * 2 + (core + n) % 2

    def behind(n):
        return ((z - dz[n // 2] + chips) % chips) * 2 + (core + n) % 2

    barrier = pltpu.get_barrier_semaphore()

    def along(step, dc):
        return ((z + step + chips) % chips) * 2 + (core + dc) % 2

    near = [(along(step, dc), tp) for step in range(-4, 5) for dc in range(2) if (step, dc) != (0, 0)]
    plane = [[partner(axis, parity, y, x) for axis, parity in ORDERS[q]] for q in range(4)]
    near += [(ep, at[0] * 4 + at[1]) for at in plane[0]]
    for device in near:
        pl.semaphore_signal(barrier, inc=1, device_id=device, device_id_type=MESH)

    small_loads = [
        pltpu.make_async_copy(src, dst, op_sem.at[i])
        for i, (src, dst) in enumerate(
            ((routes_hbm, routes_ref), (tok_hbm, tok_ref), (gain_hbm, gain_ref), (rw_hbm, rw_ref), (fg_hbm, fg_ref))
        )
    ]
    for load in small_loads:
        load.start()
    loads = (
        pltpu.make_async_copy(wg_hbm.at[0], w1.at[:, pl.ds(0, hidden_units)], w_sem.at[0]),
        pltpu.make_async_copy(wu_hbm.at[0], w1.at[:, pl.ds(hidden_units, hidden_units)], w_sem.at[1]),
        pltpu.make_async_copy(wd_hbm.at[0], wd, w_sem.at[2]),
    )
    for load in loads:
        load.start()

    prep = jax.named_scope("prep")
    prep.__enter__()
    for load in small_loads:
        load.wait()
    expert = lax.broadcasted_iota(jnp.int32, (experts, tokens), 0)
    hit0 = jnp.where(routes_ref[0:1, :] == expert, 1.0, 0.0).astype(F32)
    hit1 = jnp.where(routes_ref[1:2, :] == expert, 1.0, 0.0).astype(F32)
    above = jnp.where(
        lax.broadcasted_iota(jnp.int32, (tokens, tokens), 0) < lax.broadcasted_iota(jnp.int32, (tokens, tokens), 1),
        1.0,
        0.0,
    ).astype(BF)
    before = jnp.dot((hit0 + hit1).astype(BF), above, preferred_element_type=F32)
    base = before + expert.astype(F32) * cap
    target0 = jnp.sum(hit0 * base, axis=0, keepdims=True)
    target1 = jnp.sum(hit1 * base, axis=0, keepdims=True)
    piece = 256
    for start in range(0, experts * cap, piece):
        slot = (lax.broadcasted_iota(jnp.int32, (piece, tokens), 0) + start).astype(F32)
        pick = jnp.where((slot == target0) | (slot == target1), 1.0, 0.0).astype(BF)
        picked = jnp.dot(pick, tok_ref[...], preferred_element_type=F32).astype(BF)
        outbox[pl.ds(start // cap, piece // cap)] = picked.reshape(piece // cap, cap, LANES)
    mine = [block_index(q, y, x) for q in range(4)]
    theirs = [[block_index(q, *at) for at in plane[q]] for q in range(4)]
    gains[pl.ds(mine[0], 1)] = gain_ref[...].astype(F32).reshape(1, 1, LANES)
    prep.__exit__(None, None, None)

    with jax.named_scope("barrier"):
        pl.semaphore_wait(barrier, len(near))

    gather[0, pl.ds(mine[0], 1), pl.ds(0, cap)] = outbox[pl.ds(ep, 1)]

    def dispatch(n):
        item = n // SOURCES
        pltpu.make_async_remote_copy(
            src_ref=outbox.at[ahead(n)],
            dst_ref=gather.at[item, mine[item % 4], pl.ds(n % SOURCES * cap, cap)],
            send_sem=disp_send,
            recv_sem=disp_recv.at[item // 4],
            device_id=(ahead(n), tp),
            device_id_type=MESH,
        ).start()

    def dispatch_round(k):
        for n in range(4 * SOURCES * k, 4 * SOURCES * (k + 1)):
            if n > 0:
                dispatch(n)

    close = 4 // SOURCES
    for k in range(close):
        dispatch_round(k)
    for way, step in enumerate((-4, 4)):
        pl.semaphore_signal(entered.at[way], inc=1, device_id=(along(step, 0), tp), device_id_type=MESH)

    with jax.named_scope("weights"):
        line = lax.broadcasted_iota(jnp.int32, (LANES, tokens), 0)
        stacked = jnp.where(line == 0, target0, jnp.where(line == 1, target1, 0.0))
        stacked = jnp.where(line == 2, rw_ref[0:1, :], jnp.where(line == 3, rw_ref[1:2, :], stacked))
        columns = jnp.transpose(stacked)
        slot = lax.broadcasted_iota(jnp.int32, (tokens, experts * cap), 1).astype(F32)
        mix = jnp.where(slot == columns[:, 0:1], columns[:, 2:3], 0.0)
        mix = mix + jnp.where(slot == columns[:, 1:2], columns[:, 3:4], 0.0)
        upper = mix.astype(BF)
        high[...] = upper
        low[...] = (mix - upper.astype(F32)).astype(BF)
    with jax.named_scope("hear"):
        for way in range(2):
            pl.semaphore_wait(entered.at[way], 1)
    for k in range(rounds - 1, close - 1, -1):
        dispatch_round(k)

    def all_of(ref, sem):
        pltpu.make_async_copy(ref, ref, sem).wait()

    def square_copy(off):
        return pltpu.make_async_remote_copy(
            src_ref=squares.at[tp],
            dst_ref=squares.at[tp],
            send_sem=sq_send,
            recv_sem=sq_recv,
            device_id=(ep, (tp + off) % 16),
            device_id_type=MESH,
        )

    def across(q, bit, src, dst, send_sem, recv_sem):
        at = plane[q][bit]
        pltpu.make_async_remote_copy(
            src_ref=src,
            dst_ref=dst,
            send_sem=send_sem,
            recv_sem=recv_sem,
            device_id=(ep, at[0] * 4 + at[1]),
            device_id_type=MESH,
        ).start()

    def gather_stage(k, stage):
        if stage == 0:
            sources = 4 * SOURCES - (1 if k == 0 else 0)
            all_of(outbox.at[pl.ds(0, sources)], disp_recv.at[k])
        for q in range(4):
            item = 4 * k + q
            if stage == 0:
                blocks = gather.at[item, pl.ds(mine[q], 1)]
            else:
                all_of(gather.at[item, pl.ds(0, 2 ** (stage - 1))], ag_recv.at[item, stage - 1])
                blocks = gather.at[item, pl.ds(handed_on(mine[q], stage - 1), 2 ** (stage - 1))]
            for bit in range(stage, 4):
                across(q, bit, blocks, blocks, ag_send, ag_recv.at[item, bit])
        if k == 0:
            if stage > 0:
                all_of(gains.at[pl.ds(0, 2 ** (stage - 1))], gain_recv.at[stage - 1])
            group = gains.at[pl.ds((mine[0] // 2**stage) * 2**stage, 2**stage)]
            across(0, stage, group, group, gain_send, gain_recv.at[stage])

    def scatter_send(item, stage):
        bit = 3 - stage
        q = item % 4
        other = theirs[q][bit]
        for step in range(stage + 1, 5):
            start = landing(stage, step)
            size = 2 ** (3 - step) if step < 4 else 1
            block = handed_on(other, 3 - step) if step < 4 else other
            across(
                q,
                bit,
                parts.at[item, pl.ds(block, size)],
                inbound[stage].at[item, pl.ds(start, size)],
                rs_send,
                rs_recv.at[item, step - 1],
            )

    def give_back(n):
        pltpu.make_async_remote_copy(
            src_ref=done.at[n // SOURCES, pl.ds(n % SOURCES * cap, cap)],
            dst_ref=returned.at[ep],
            send_sem=ret_send,
            recv_sem=ret_recv,
            device_id=(behind(n), tp),
            device_id_type=MESH,
        ).start()

    first = [k for k, stage in ORDER if stage == 4][0]

    def experts_stage(k):
        for q in range(4):
            all_of(gather.at[4 * k + q, pl.ds(0, 8)], ag_recv.at[4 * k + q, 3])
        if k == first:
            all_of(gains.at[pl.ds(0, 8)], gain_recv.at[3])
            for load in loads:
                load.wait()
        for q in range(4):
            item = 4 * k + q
            total = jnp.zeros((rows, LANES), F32)
            for t in range(16):
                row = gather[item, block_index(q, t // 4, t % 4)].astype(F32)
                total = total + row * row
            scale = lax.rsqrt(jnp.sum(total, axis=1, keepdims=True) / width + EPS)
            scale = jnp.broadcast_to(scale, (rows, LANES))
            for t in range(16):
                row = gather[item, block_index(q, t // 4, t % 4)].astype(F32)
                normed[pl.ds(q * rows, rows), pl.ds(t * LANES, LANES)] = (row * scale * gains[block_index(0, t // 4, t % 4)]).astype(BF)
        both = jnp.dot(normed[...], w1[...], preferred_element_type=F32)
        gate, up = both[:, :hidden_units], both[:, hidden_units:]
        hidden = (gate / (1.0 + jnp.exp(-gate)) * up).astype(BF)
        for pair in range(8):
            part = jnp.dot(hidden, wd[:, pl.ds(pair * 256, 256)], preferred_element_type=F32).astype(BF)
            for q in range(4):
                for t in (2 * pair, 2 * pair + 1):
                    parts[4 * k + q, block_index(q, t // 4, t % 4)] = part[
                        q * rows : (q + 1) * rows, (t % 2) * LANES : (t % 2 + 1) * LANES
                    ]
        for q in range(4):
            scatter_send(4 * k + q, 0)

    def scatter_stage(k, step):
        size = 2 ** (3 - step) if step < 4 else 1
        for q in range(4):
            item = 4 * k + q
            all_of(parts.at[item, pl.ds(0, step * size)], rs_recv.at[item, step - 1])
            block = pl.ds(handed_on(mine[q], 3 - step) if step < 4 else mine[q], size)
            added = parts[item, block].astype(F32)
            for stage in range(step):
                start = landing(stage, step)
                added = added + inbound[stage][item, start : start + size].astype(F32)
            if step < 4:
                parts[item, block] = added.astype(BF)
            else:
                done[item] = added[0].astype(BF)
        for q in range(4):
            item = 4 * k + q
            if step < 4:
                scatter_send(item, step)
            else:
                for n in range(SOURCES * item, SOURCES * (item + 1)):
                    if n == 0:
                        returned[pl.ds(ep, 1)] = done[0, pl.ds(0, cap)].reshape(1, cap, LANES)
                    else:
                        give_back(n)

    for k, stage in ORDER:
        with jax.named_scope("r%d_s%d" % (k, stage)):
            if stage < 4:
                gather_stage(k, stage)
            elif stage == 4:
                experts_stage(k)
            else:
                scatter_stage(k, stage - 4)

    all_of(outbox.at[pl.ds(0, experts - 1)], disp_send)
    all_of(gains.at[pl.ds(0, 15)], gain_send)
    all_of(gather.at[:, pl.ds(0, 15)], ag_send)
    all_of(parts.at[:, pl.ds(0, 15)], rs_send)
    with jax.named_scope("retwait"):
        all_of(returned.at[pl.ds(0, experts - 1)], ret_recv)
    with jax.named_scope("combine"):
        results = returned[...].reshape(experts * cap, LANES)
        combined = jnp.dot(high[...], results, preferred_element_type=F32)
        combined = combined + jnp.dot(low[...], results, preferred_element_type=F32)
        square = jnp.sum(jnp.transpose(combined * combined), axis=0, keepdims=True)
        squares[pl.ds(tp, 1)] = square.reshape(1, 1, tokens)
        for off in range(1, 16):
            square_copy(off).start()
    all_of(outbox.at[pl.ds(0, experts - 1)], ret_send)
    with jax.named_scope("sqwait"):
        all_of(squares.at[pl.ds(0, 15)], sq_recv)
    total = squares[0]
    for t in range(1, 16):
        total = total + squares[t]
    final = lax.rsqrt(total / width + EPS)
    final = jnp.transpose(jnp.broadcast_to(final, (LANES, tokens)))
    out_ref[...] = (combined * final * fg_ref[...].astype(F32)).astype(BF)

    all_of(squares.at[pl.ds(0, 15)], sq_send)


def local(tokens, norm_gain, w_gate, w_up, w_down, routes, route_weights, final_gain):
    experts = lax.axis_size("ep")
    chips = experts // 2
    items = experts // SOURCES
    tok_rows, share = tokens.shape
    cap = 2 * tok_rows * routes.shape[1] // experts
    hidden_units = w_gate.shape[2]
    rows = SOURCES * cap
    vmem = pl.BlockSpec(memory_space=pltpu.VMEM)
    hbm = pl.BlockSpec(memory_space=pl.ANY)
    dma = pltpu.SemaphoreType.DMA
    return pl.pallas_call(
        functools.partial(body, chips),
        out_shape=jax.ShapeDtypeStruct((tok_rows, share), BF),
        in_specs=[hbm] * 8,
        out_specs=vmem,
        scratch_shapes=[
            pltpu.VMEM((16 * share, 2 * hidden_units), BF),
            pltpu.VMEM((hidden_units, 16 * share), BF),
            pltpu.VMEM((experts, cap, share), BF),
            pltpu.VMEM((items, 16, rows, share), BF),
            pltpu.VMEM((4 * rows, 16 * share), BF),
            pltpu.VMEM((items, 16, rows, share), BF),
            pltpu.VMEM((items, 8, rows, share), BF),
            pltpu.VMEM((items, 4, rows, share), BF),
            pltpu.VMEM((items, 2, rows, share), BF),
            pltpu.VMEM((items, 1, rows, share), BF),
            pltpu.VMEM((items, rows, share), BF),
            pltpu.VMEM((experts, cap, share), BF),
            pltpu.VMEM((16, 1, share), F32),
            pltpu.VMEM((16, 1, tok_rows), F32),
            dma((3,)),
            dma,
            dma((items // 4,)),
            dma,
            dma((items, 4)),
            dma,
            dma((items, 4)),
            dma,
            dma,
            dma,
            dma((4,)),
            dma,
            dma,
            pltpu.VMEM((tok_rows, experts * cap), BF),
            pltpu.VMEM((tok_rows, experts * cap), BF),
            pltpu.SemaphoreType.REGULAR((2,)),
            pltpu.VMEM((tok_rows, share), BF),
            pltpu.VMEM((1, share), BF),
            pltpu.VMEM((2, tok_rows), jnp.int32),
            pltpu.VMEM((2, tok_rows), F32),
            pltpu.VMEM((1, share), BF),
            dma((5,)),
        ],
        compiler_params=pltpu.CompilerParams(collective_id=0, has_side_effects=True),
    )(
        tokens,
        norm_gain.reshape(1, -1),
        routes.T,
        route_weights.T,
        final_gain.reshape(1, -1),
        w_gate,
        w_up,
        w_down,
    )


def solution(mesh):
    in_specs = (
        P("ep", "tp"),
        P("tp"),
        P("ep", None, "tp"),
        P("ep", None, "tp"),
        P("ep", "tp", None),
        P("ep", None),
        P("ep", None),
        P("tp"),
    )
    out_specs = P("ep", "tp")
    return jax.shard_map(local, mesh=mesh, in_specs=in_specs, out_specs=out_specs, check_vma=False)
```

```python
import functools

import jax
import jax.numpy as jnp
from jax import lax
from jax.experimental import pallas as pl
from jax.experimental.pallas import tpu as pltpu
from jax.sharding import PartitionSpec as P

EPS = 1e-06
LANES = 128
MESH = pl.DeviceIdType.MESH
BF, F32 = jnp.bfloat16, jnp.float32

ORDERS = (
    (("x", 0), ("y", 0), ("x", 1), ("y", 1)),
    (("y", 0), ("x", 1), ("y", 1), ("x", 0)),
    (("x", 1), ("y", 1), ("x", 0), ("y", 0)),
    (("y", 1), ("x", 0), ("y", 0), ("x", 1)),
)
ORDER = (
    (0, 0), (1, 0), (0, 1), (1, 1), (0, 2), (3, 0), (2, 0), (0, 3), (3, 1), (2, 1), (1, 2), (3, 2),
    (2, 2), (1, 3), (3, 3), (2, 3), (0, 4), (3, 4), (2, 4), (3, 5), (1, 4), (3, 6), (2, 5), (1, 5),
    (3, 7), (2, 6), (0, 5), (1, 6), (3, 8), (2, 7), (0, 6), (1, 7), (2, 8), (0, 7), (1, 8), (0, 8),
)
SOURCES = 2


def block_index(quarter, y, x):
    place = {}
    index = 0
    seen = {"x": 0, "y": 0}
    for bit, (axis, parity) in enumerate(ORDERS[quarter]):
        at = x if axis == "x" else y
        if seen[axis] == 0:
            place[axis] = (at + parity) % 4
            index = index + (place[axis] % 2) * 2**bit
        else:
            index = index + (place[axis] // 2) * 2**bit
        seen[axis] += 1
    return index


def partner(axis, parity, y, x):
    at = x if axis == "x" else y
    step = 1 - 2 * ((at + parity) % 2)
    other = (at + step + 4) % 4
    return (y, other) if axis == "x" else (other, x)


def handed_on(index, bit):
    return (index // 2 ** (bit + 1)) * 2 ** (bit + 1) + (1 - (index // 2**bit) % 2) * 2**bit


def landing(stage, step):
    return 2 ** (3 - stage) - (2 ** (4 - step))


def distances(chips):
    out = [0]
    for d in range(1, chips // 2 + 1):
        out.append(d)
        if d != chips - d:
            out.append(-d)
    return out


def body(
    chips,
    tok_hbm,
    gain_hbm,
    routes_hbm,
    rw_hbm,
    fg_hbm,
    wg_hbm,
    wu_hbm,
    wd_hbm,
    out_ref,
    w1,
    wd,
    outbox,
    gather,
    normed,
    parts,
    in0,
    in1,
    in2,
    in3,
    done,
    returned,
    gains,
    squares,
    w_sem,
    disp_send,
    disp_recv,
    ag_send,
    ag_recv,
    rs_send,
    rs_recv,
    ret_send,
    ret_recv,
    gain_send,
    gain_recv,
    sq_send,
    sq_recv,
    high,
    low,
    entered,
    tok_ref,
    gain_ref,
    routes_ref,
    rw_ref,
    fg_ref,
    op_sem,
):
    inbound = (in0, in1, in2, in3)
    ep, tp = lax.axis_index("ep"), lax.axis_index("tp")
    z, core = ep // 2, ep % 2
    y, x = tp // 4, tp % 4
    tokens = tok_ref.shape[0]
    experts, cap = outbox.shape[0], outbox.shape[1]
    items = experts // SOURCES
    rounds = items // 4
    rows = SOURCES * cap
    width = 16 * LANES
    hidden_units = wd.shape[0]
    dz = distances(chips)

    def ahead(n):
        return ((z + dz[n // 2] + chips) % chips) * 2 + (core + n) % 2

    def behind(n):
        return ((z - dz[n // 2] + chips) % chips) * 2 + (core + n) % 2

    barrier = pltpu.get_barrier_semaphore()

    def along(step, dc):
        return ((z + step + chips) % chips) * 2 + (core + dc) % 2

    near = [(along(step, dc), tp) for step in range(-4, 5) for dc in range(2) if (step, dc) != (0, 0)]
    plane = [[partner(axis, parity, y, x) for axis, parity in ORDERS[q]] for q in range(4)]
    near += [(ep, at[0] * 4 + at[1]) for at in plane[0]]
    for device in near:
        pl.semaphore_signal(barrier, inc=1, device_id=device, device_id_type=MESH)

    small_loads = [
        pltpu.make_async_copy(src, dst, op_sem.at[i])
        for i, (src, dst) in enumerate(
            ((routes_hbm, routes_ref), (tok_hbm, tok_ref), (gain_hbm, gain_ref), (rw_hbm, rw_ref), (fg_hbm, fg_ref))
        )
    ]
    for load in small_loads:
        load.start()
    loads = (
        pltpu.make_async_copy(wg_hbm.at[0], w1.at[:, pl.ds(0, hidden_units)], w_sem.at[0]),
        pltpu.make_async_copy(wu_hbm.at[0], w1.at[:, pl.ds(hidden_units, hidden_units)], w_sem.at[1]),
        pltpu.make_async_copy(wd_hbm.at[0], wd, w_sem.at[2]),
    )
    for load in loads:
        load.start()

    prep = jax.named_scope("prep")
    prep.__enter__()
    for load in small_loads:
        load.wait()
    expert = lax.broadcasted_iota(jnp.int32, (experts, tokens), 0)
    hit0 = jnp.where(routes_ref[0:1, :] == expert, 1.0, 0.0).astype(F32)
    hit1 = jnp.where(routes_ref[1:2, :] == expert, 1.0, 0.0).astype(F32)
    above = jnp.where(
        lax.broadcasted_iota(jnp.int32, (tokens, tokens), 0) < lax.broadcasted_iota(jnp.int32, (tokens, tokens), 1),
        1.0,
        0.0,
    ).astype(BF)
    before = jnp.dot((hit0 + hit1).astype(BF), above, preferred_element_type=F32)
    base = before + expert.astype(F32) * cap
    target0 = jnp.sum(hit0 * base, axis=0, keepdims=True)
    target1 = jnp.sum(hit1 * base, axis=0, keepdims=True)
    piece = 256
    for start in range(0, experts * cap, piece):
        slot = (lax.broadcasted_iota(jnp.int32, (piece, tokens), 0) + start).astype(F32)
        pick = jnp.where((slot == target0) | (slot == target1), 1.0, 0.0).astype(BF)
        picked = jnp.dot(pick, tok_ref[...], preferred_element_type=F32).astype(BF)
        outbox[pl.ds(start // cap, piece // cap)] = picked.reshape(piece // cap, cap, LANES)
    mine = [block_index(q, y, x) for q in range(4)]
    theirs = [[block_index(q, *at) for at in plane[q]] for q in range(4)]
    gains[pl.ds(mine[0], 1)] = gain_ref[...].astype(F32).reshape(1, 1, LANES)
    prep.__exit__(None, None, None)

    with jax.named_scope("barrier"):
        pl.semaphore_wait(barrier, len(near))

    gather[0, pl.ds(mine[0], 1), pl.ds(0, cap)] = outbox[pl.ds(ep, 1)]

    def dispatch(n):
        item = n // SOURCES
        pltpu.make_async_remote_copy(
            src_ref=outbox.at[ahead(n)],
            dst_ref=gather.at[item, mine[item % 4], pl.ds(n % SOURCES * cap, cap)],
            send_sem=disp_send,
            recv_sem=disp_recv.at[item // 4],
            device_id=(ahead(n), tp),
            device_id_type=MESH,
        ).start()

    close = 4 // SOURCES

    def dispatch_round(k):
        order = range(4 * SOURCES * k, 4 * SOURCES * (k + 1))
        for n in order if k < close else reversed(order):
            if n > 0:
                dispatch(n)

    for way, step in enumerate((-4, 4)):
        pl.semaphore_signal(entered.at[way], inc=1, device_id=(along(step, 0), tp), device_id_type=MESH)
    dispatch_round(0)

    with jax.named_scope("weights"):
        line = lax.broadcasted_iota(jnp.int32, (LANES, tokens), 0)
        stacked = jnp.where(line == 0, target0, jnp.where(line == 1, target1, 0.0))
        stacked = jnp.where(line == 2, rw_ref[0:1, :], jnp.where(line == 3, rw_ref[1:2, :], stacked))
        columns = jnp.transpose(stacked)
        slot = lax.broadcasted_iota(jnp.int32, (tokens, experts * cap), 1).astype(F32)
        mix = jnp.where(slot == columns[:, 0:1], columns[:, 2:3], 0.0)
        mix = mix + jnp.where(slot == columns[:, 1:2], columns[:, 3:4], 0.0)
        upper = mix.astype(BF)
        high[...] = upper
        low[...] = (mix - upper.astype(F32)).astype(BF)
    for k in range(1, close):
        dispatch_round(k)
    with jax.named_scope("hear"):
        for way in range(2):
            pl.semaphore_wait(entered.at[way], 1)
    for k in range(rounds - 1, close - 1, -1):
        dispatch_round(k)

    def all_of(ref, sem):
        pltpu.make_async_copy(ref, ref, sem).wait()

    def square_copy(off):
        return pltpu.make_async_remote_copy(
            src_ref=squares.at[tp],
            dst_ref=squares.at[tp],
            send_sem=sq_send,
            recv_sem=sq_recv,
            device_id=(ep, (tp + off) % 16),
            device_id_type=MESH,
        )

    def across(q, bit, src, dst, send_sem, recv_sem):
        at = plane[q][bit]
        pltpu.make_async_remote_copy(
            src_ref=src,
            dst_ref=dst,
            send_sem=send_sem,
            recv_sem=recv_sem,
            device_id=(ep, at[0] * 4 + at[1]),
            device_id_type=MESH,
        ).start()

    def gather_stage(k, stage):
        if stage == 0:
            sources = 4 * SOURCES - (1 if k == 0 else 0)
            all_of(outbox.at[pl.ds(0, sources)], disp_recv.at[k])
        for q in range(4):
            item = 4 * k + q
            if stage == 0:
                blocks = gather.at[item, pl.ds(mine[q], 1)]
            else:
                all_of(gather.at[item, pl.ds(0, 2 ** (stage - 1))], ag_recv.at[item, stage - 1])
                blocks = gather.at[item, pl.ds(handed_on(mine[q], stage - 1), 2 ** (stage - 1))]
            for bit in range(stage, 4):
                across(q, bit, blocks, blocks, ag_send, ag_recv.at[item, bit])
        if k == 0:
            if stage > 0:
                all_of(gains.at[pl.ds(0, 2 ** (stage - 1))], gain_recv.at[stage - 1])
            group = gains.at[pl.ds((mine[0] // 2**stage) * 2**stage, 2**stage)]
            across(0, stage, group, group, gain_send, gain_recv.at[stage])

    def scatter_send(item, stage):
        bit = 3 - stage
        q = item % 4
        other = theirs[q][bit]
        for step in range(stage + 1, 5):
            start = landing(stage, step)
            size = 2 ** (3 - step) if step < 4 else 1
            block = handed_on(other, 3 - step) if step < 4 else other
            across(
                q,
                bit,
                parts.at[item, pl.ds(block, size)],
                inbound[stage].at[item, pl.ds(start, size)],
                rs_send,
                rs_recv.at[item, step - 1],
            )

    def give_back(n):
        pltpu.make_async_remote_copy(
            src_ref=done.at[n // SOURCES, pl.ds(n % SOURCES * cap, cap)],
            dst_ref=returned.at[ep],
            send_sem=ret_send,
            recv_sem=ret_recv,
            device_id=(behind(n), tp),
            device_id_type=MESH,
        ).start()

    first = [k for k, stage in ORDER if stage == 4][0]

    def experts_stage(k):
        for q in range(4):
            all_of(gather.at[4 * k + q, pl.ds(0, 8)], ag_recv.at[4 * k + q, 3])
        if k == first:
            all_of(gains.at[pl.ds(0, 8)], gain_recv.at[3])
            for load in loads:
                load.wait()
        for q in range(4):
            item = 4 * k + q
            total = jnp.zeros((rows, LANES), F32)
            for t in range(16):
                row = gather[item, block_index(q, t // 4, t % 4)].astype(F32)
                total = total + row * row
            scale = lax.rsqrt(jnp.sum(total, axis=1, keepdims=True) / width + EPS)
            scale = jnp.broadcast_to(scale, (rows, LANES))
            for t in range(16):
                row = gather[item, block_index(q, t // 4, t % 4)].astype(F32)
                normed[pl.ds(q * rows, rows), pl.ds(t * LANES, LANES)] = (row * scale * gains[block_index(0, t // 4, t % 4)]).astype(BF)
        both = jnp.dot(normed[...], w1[...], preferred_element_type=F32)
        gate, up = both[:, :hidden_units], both[:, hidden_units:]
        hidden = (gate / (1.0 + jnp.exp(-gate)) * up).astype(BF)
        for pair in range(8):
            part = jnp.dot(hidden, wd[:, pl.ds(pair * 256, 256)], preferred_element_type=F32).astype(BF)
            for q in range(4):
                for t in (2 * pair, 2 * pair + 1):
                    parts[4 * k + q, block_index(q, t // 4, t % 4)] = part[
                        q * rows : (q + 1) * rows, (t % 2) * LANES : (t % 2 + 1) * LANES
                    ]
        for q in range(4):
            scatter_send(4 * k + q, 0)

    def scatter_stage(k, step):
        size = 2 ** (3 - step) if step < 4 else 1
        for q in range(4):
            item = 4 * k + q
            all_of(parts.at[item, pl.ds(0, step * size)], rs_recv.at[item, step - 1])
            block = pl.ds(handed_on(mine[q], 3 - step) if step < 4 else mine[q], size)
            added = parts[item, block].astype(F32)
            for stage in range(step):
                start = landing(stage, step)
                added = added + inbound[stage][item, start : start + size].astype(F32)
            if step < 4:
                parts[item, block] = added.astype(BF)
            else:
                done[item] = added[0].astype(BF)
        for q in range(4) if step < 4 else reversed(range(4)):
            item = 4 * k + q
            if step < 4:
                scatter_send(item, step)
            else:
                for n in range(SOURCES * item, SOURCES * (item + 1)):
                    if n == 0:
                        returned[pl.ds(ep, 1)] = done[0, pl.ds(0, cap)].reshape(1, cap, LANES)
                    else:
                        give_back(n)

    for k, stage in ORDER:
        with jax.named_scope("r%d_s%d" % (k, stage)):
            if stage < 4:
                gather_stage(k, stage)
            elif stage == 4:
                experts_stage(k)
            else:
                scatter_stage(k, stage - 4)

    all_of(outbox.at[pl.ds(0, experts - 1)], disp_send)
    all_of(gains.at[pl.ds(0, 15)], gain_send)
    all_of(gather.at[:, pl.ds(0, 15)], ag_send)
    all_of(parts.at[:, pl.ds(0, 15)], rs_send)
    with jax.named_scope("retwait"):
        all_of(returned.at[pl.ds(0, experts - 1)], ret_recv)
    with jax.named_scope("combine"):
        results = returned[...].reshape(experts * cap, LANES)
        combined = jnp.dot(high[...], results, preferred_element_type=F32)
        combined = combined + jnp.dot(low[...], results, preferred_element_type=F32)
        square = jnp.sum(jnp.transpose(combined * combined), axis=0, keepdims=True)
        squares[pl.ds(tp, 1)] = square.reshape(1, 1, tokens)
        for off in range(1, 16):
            square_copy(off).start()
    all_of(outbox.at[pl.ds(0, experts - 1)], ret_send)
    with jax.named_scope("sqwait"):
        all_of(squares.at[pl.ds(0, 15)], sq_recv)
    total = squares[0]
    for t in range(1, 16):
        total = total + squares[t]
    final = lax.rsqrt(total / width + EPS)
    final = jnp.transpose(jnp.broadcast_to(final, (LANES, tokens)))
    out_ref[...] = (combined * final * fg_ref[...].astype(F32)).astype(BF)

    all_of(squares.at[pl.ds(0, 15)], sq_send)


def local(tokens, norm_gain, w_gate, w_up, w_down, routes, route_weights, final_gain):
    experts = lax.axis_size("ep")
    chips = experts // 2
    items = experts // SOURCES
    tok_rows, share = tokens.shape
    cap = 2 * tok_rows * routes.shape[1] // experts
    hidden_units = w_gate.shape[2]
    rows = SOURCES * cap
    vmem = pl.BlockSpec(memory_space=pltpu.VMEM)
    hbm = pl.BlockSpec(memory_space=pl.ANY)
    dma = pltpu.SemaphoreType.DMA
    return pl.pallas_call(
        functools.partial(body, chips),
        out_shape=jax.ShapeDtypeStruct((tok_rows, share), BF),
        in_specs=[hbm] * 8,
        out_specs=vmem,
        scratch_shapes=[
            pltpu.VMEM((16 * share, 2 * hidden_units), BF),
            pltpu.VMEM((hidden_units, 16 * share), BF),
            pltpu.VMEM((experts, cap, share), BF),
            pltpu.VMEM((items, 16, rows, share), BF),
            pltpu.VMEM((4 * rows, 16 * share), BF),
            pltpu.VMEM((items, 16, rows, share), BF),
            pltpu.VMEM((items, 8, rows, share), BF),
            pltpu.VMEM((items, 4, rows, share), BF),
            pltpu.VMEM((items, 2, rows, share), BF),
            pltpu.VMEM((items, 1, rows, share), BF),
            pltpu.VMEM((items, rows, share), BF),
            pltpu.VMEM((experts, cap, share), BF),
            pltpu.VMEM((16, 1, share), F32),
            pltpu.VMEM((16, 1, tok_rows), F32),
            dma((3,)),
            dma,
            dma((items // 4,)),
            dma,
            dma((items, 4)),
            dma,
            dma((items, 4)),
            dma,
            dma,
            dma,
            dma((4,)),
            dma,
            dma,
            pltpu.VMEM((tok_rows, experts * cap), BF),
            pltpu.VMEM((tok_rows, experts * cap), BF),
            pltpu.SemaphoreType.REGULAR((2,)),
            pltpu.VMEM((tok_rows, share), BF),
            pltpu.VMEM((1, share), BF),
            pltpu.VMEM((2, tok_rows), jnp.int32),
            pltpu.VMEM((2, tok_rows), F32),
            pltpu.VMEM((1, share), BF),
            dma((5,)),
        ],
        compiler_params=pltpu.CompilerParams(collective_id=0, has_side_effects=True),
    )(
        tokens,
        norm_gain.reshape(1, -1),
        routes.T,
        route_weights.T,
        final_gain.reshape(1, -1),
        w_gate,
        w_up,
        w_down,
    )


def solution(mesh):
    in_specs = (
        P("ep", "tp"),
        P("tp"),
        P("ep", None, "tp"),
        P("ep", None, "tp"),
        P("ep", "tp", None),
        P("ep", None),
        P("ep", None),
        P("tp"),
    )
    out_specs = P("ep", "tp")
    return jax.shard_map(local, mesh=mesh, in_specs=in_specs, out_specs=out_specs, check_vma=False)
```
